256 devices in a mesh: grp: 2 (over y), sp: 16 (over z), tp: 8 (over x, core).
Axes of the slice: x: 4, y: 2, z: 16, core: 2. Of those that a mesh axis runs over, the one named last changes fastest.
The devices are a block of a 4x16x16 slice.
Arguments:
- queries: bfloat16 [16384, 1024], P(('grp', 'sp'), 'tp'), parts along dimension 0, may hold values from -5 to 9
- keys: bfloat16 [16384, 1024], P(('grp', 'sp'), 'tp'), parts along dimension 0, may hold values from -12 to 5
- values: bfloat16 [16384, 1024], P(('grp', 'sp'), 'tp'), parts along dimension 0, may hold values from -5 to 5
- residual: bfloat16 [16384, 2048], P(('grp', 'sp')), parts along dimension 0, may hold values from -6 to 6
- out_weight: bfloat16 [1024, 2048], P('tp'), may hold values from -0.1875 to 0.1875
- post_gain: float32 [2048], replicated, may hold values from 0.1 to 1.9
- gate_weight: bfloat16 [2048, 5120], P('sp', 'tp'), may hold values from -0.125 to 0.125
- up_weight: bfloat16 [2048, 5120], P('sp', 'tp'), may hold values from -0.125 to 0.125
- down_weight: bfloat16 [5120, 2048], P('tp', 'sp'), may hold values from -0.078125 to 0.078125
- ffn_pre_gain: float32 [2048], replicated, may hold values from 0.1 to 1.9
- ffn_post_gain: float32 [2048], replicated, may hold values from 0.1 to 1.9
Outputs:
- layer_out: bfloat16 [16384, 2048], P(('grp', 'sp', 'tp')), parts along dimension 0
The draws below stay inside these ranges and needn't reach their ends.
There are 2 independent parts, one for each index of `grp`. The reference program is written for one: setup_inputs(seed, part) draws one part's arguments, and reference() takes and returns one part's arrays. A program takes and returns all parts, laid end to end along the dimension named above; an argument that names none is the same for every part. Nothing has to cross between parts.
All inputs are finite; a program needn't handle non-finite values.
Results may differ from the reference program's by a relative error of at most 0.014.
Values may be sent and summed in bfloat16 or wider, within the bound.
A program may use at most 64 MiB of HBM per device.

```python
import math
import jax
import jax.numpy as jnp
from jax import lax

D = 2048
HEAD_TOTAL = 16
HEAD_DIM = 64
FF = 5120
TOK_DEV = 512
TOKEN_TOTAL = 8192
N_TP = 8


def draw_queries(key, part):
    noise_random_key, lead_key = jax.random.split(key)
    noise = jnp.clip(jax.random.normal(noise_random_key, (TOKEN_TOTAL, HEAD_TOTAL, HEAD_DIM), jnp.float32), -5.0, 5.0)
    leader_value = jax.random.uniform(lead_key, (TOKEN_TOTAL, HEAD_TOTAL), jnp.float32, 0.875, 1.125) * math.sqrt(HEAD_DIM)
    lead_mask = jnp.arange(HEAD_DIM) == 0
    drawn = jnp.where(lead_mask[None, None, :], leader_value[:, :, None], noise)
    return drawn.reshape(TOKEN_TOTAL, HEAD_TOTAL * HEAD_DIM).astype(jnp.bfloat16)


def draw_keys(key, part):
    split_keys = jax.random.split(key, 7)
    noise_random_key = split_keys[0]
    velocity_random_key = split_keys[1]
    block_random_key = split_keys[2]
    spike_random_key = split_keys[3]
    position_random_key = split_keys[4]
    middle_pick_key = split_keys[5]
    middle_value_key = split_keys[6]
    noise = jnp.clip(jax.random.normal(noise_random_key, (TOKEN_TOTAL, HEAD_TOTAL, HEAD_DIM), jnp.float32), -5.0, 5.0)
    fast_head = jax.random.uniform(velocity_random_key, (HEAD_TOTAL,), jnp.float32) < 0.5
    chain_rate = math.log(TOKEN_TOTAL) + 1.0
    head_rate = jnp.where(fast_head, 3.5, chain_rate)
    blocks = TOKEN_TOTAL // TOK_DEV
    block_shift = jax.random.uniform(block_random_key, (blocks,), jnp.float32, -0.92, 0.92)
    shift_rows = jnp.repeat(block_shift, TOK_DEV)
    leader_value = shift_rows[:, None] - head_rate[None, :]
    middle_picks = jax.random.randint(middle_pick_key, (blocks, 2, HEAD_TOTAL), 0, TOK_DEV)
    middle_rows = jnp.repeat(middle_picks, TOK_DEV, axis=0)
    row_in_block = jnp.arange(TOKEN_TOTAL) % TOK_DEV
    middle_mask = jnp.any(row_in_block[:, None, None] == middle_rows, axis=1)
    middle_mask = jnp.logical_and(middle_mask, jnp.logical_not(fast_head)[None, :])
    middle_value = jax.random.uniform(middle_value_key, (TOKEN_TOTAL, HEAD_TOTAL), jnp.float32, -4.5, -3.0)
    leader_value = jnp.where(middle_mask, middle_value, leader_value)
    spike_row_indices = jax.random.randint(position_random_key, (4,), 0, TOKEN_TOTAL)
    spike_present = jnp.any(jnp.arange(TOKEN_TOTAL)[:, None] == spike_row_indices[None, :], axis=1)
    spike_leader = -jax.random.uniform(spike_random_key, (TOKEN_TOTAL, HEAD_TOTAL), jnp.float32, 0.0, 1.4)
    leader_value = jnp.where(spike_present[:, None], spike_leader, leader_value)
    lead_mask = jnp.arange(HEAD_DIM) == 0
    drawn = jnp.where(lead_mask[None, None, :], leader_value[:, :, None], noise)
    return drawn.reshape(TOKEN_TOTAL, HEAD_TOTAL * HEAD_DIM).astype(jnp.bfloat16)


def block_levels(own_key, extent, pieces, least, top_value):
    level, own = 1.0, jax.random.fold_in(own_key, 6)
    for dim, shards_of in pieces:
        draws = jnp.exp(jax.random.uniform(jax.random.fold_in(own, dim), (shards_of,), jnp.float32, least / len(pieces), top_value / len(pieces)))
        level = level * jnp.repeat(draws, extent[dim] // shards_of).reshape([-1 if axis == dim else 1 for axis in range(len(extent))])
    return level


def gaussian(own_key, extent, deviation, limit, cuts=(), held_as=jnp.bfloat16):
    entries = deviation * jax.random.normal(own_key, extent, jnp.float32)
    if cuts:
        entries = entries * block_levels(own_key, extent, cuts, -0.22, 0.18)
    return jnp.clip(entries, -limit, limit).astype(held_as)


def setup_inputs(seed: int = 0, part: int = 0) -> dict:
    key_of = jax.random.split(jax.random.key(seed), 12)
    own_keys = jax.random.split(jax.random.fold_in(key_of[11], part), 12)
    return {
        "queries": draw_queries(jax.random.fold_in(jax.random.fold_in(key_of[11], part), 71), part),
        "keys": draw_keys(jax.random.fold_in(jax.random.fold_in(key_of[11], part), 71), part),
        "values": gaussian(own_keys[2], (TOKEN_TOTAL, HEAD_TOTAL * HEAD_DIM), 1.0, 5.0, ((0, 16), (1, 8))),
        "residual": gaussian(own_keys[3], (TOKEN_TOTAL, D), 1.0, 6.0, ((0, 16),)),
        "out_weight": gaussian(key_of[4], (HEAD_TOTAL * HEAD_DIM, D), (HEAD_TOTAL * HEAD_DIM) ** -0.5, 0.1875, ((0, 8),)),
        "post_gain": jnp.clip(1.0 + 0.18 * jax.random.normal(key_of[5], (D,), jnp.float32), 0.1, 1.9),
        "gate_weight": gaussian(key_of[6], (D, FF), D ** -0.5, 0.125, ((0, 16), (1, 8))),
        "up_weight": gaussian(key_of[7], (D, FF), D ** -0.5, 0.125, ((0, 16), (1, 8))),
        "down_weight": gaussian(key_of[8], (FF, D), FF ** -0.5, 0.078125, ((0, 8), (1, 16))),
        "ffn_pre_gain": jnp.clip(1.0 + 0.18 * jax.random.normal(key_of[9], (D,), jnp.float32), 0.1, 1.9),
        "ffn_post_gain": jnp.clip(1.0 + 0.18 * jax.random.normal(key_of[10], (D,), jnp.float32), 0.1, 1.9),
    }


norm_eps = 1e-06

def rms_scale(row_block, gain):
    mean_square = lax.optimization_barrier(jnp.mean(row_block * row_block, axis=-1, keepdims=True))
    return row_block * lax.rsqrt(mean_square + norm_eps) * gain

def group_sum(left, right, group_width):
    groups = left.shape[1] // group_width

    def add_group(acc, group_index):
        left_cols = lax.dynamic_slice_in_dim(left, group_index * group_width, group_width, 1)
        right_rows = lax.dynamic_slice_in_dim(right, group_index * group_width, group_width, 0)
        partial_sum = jnp.dot(left_cols, right_rows, preferred_element_type=jnp.float32).astype(jnp.bfloat16)
        partial_sum = lax.optimization_barrier(partial_sum)
        return (acc + partial_sum.astype(jnp.float32), None)
    summed, unused = lax.scan(add_group, jnp.zeros((left.shape[0], right.shape[1]), jnp.float32), jnp.arange(groups, dtype=jnp.int32))
    return summed

def reference(queries, keys, values, residual, out_weight, post_gain, gate_weight, up_weight, down_weight, ffn_pre_gain, ffn_post_gain):
    key_total = queries.shape[0]
    key_span = math.gcd(512, key_total)
    score_scale = 1.0 / math.sqrt(HEAD_DIM)
    positions = jnp.arange(key_total, dtype=jnp.int32)
    q_heads = queries.reshape(key_total, HEAD_TOTAL, HEAD_DIM).transpose(1, 0, 2)
    k_heads = keys.reshape(key_total, HEAD_TOTAL, HEAD_DIM).transpose(1, 0, 2)
    v_heads = values.reshape(key_total, HEAD_TOTAL, HEAD_DIM).transpose(1, 0, 2)

    def stick_head(head_args):
        q_head, k_head, v_head = head_args

        def one_block(block_index):
            row_start = block_index * key_span
            q_rows = lax.dynamic_slice_in_dim(q_head, row_start, key_span, 0)
            scores = jnp.dot(q_rows, k_head.T, preferred_element_type=jnp.float32) * score_scale
            q_pos = row_start + jnp.arange(key_span, dtype=jnp.int32)
            strict = positions[None, :] < q_pos[:, None]
            fall_log = jnp.where(strict, jax.nn.log_sigmoid(-scores), 0.0)
            later_sum = lax.cumsum(fall_log, axis=1, reverse=True) - fall_log
            weights = jnp.where(strict, jnp.exp(jax.nn.log_sigmoid(scores) + later_sum), 0.0)
            return jnp.dot(weights.astype(jnp.bfloat16), v_head, preferred_element_type=jnp.float32)
        blocks_out = lax.map(one_block, jnp.arange(key_total // key_span, dtype=jnp.int32))
        return blocks_out.reshape(key_total, HEAD_DIM)
    heads_out = lax.map(stick_head, (q_heads, k_heads, v_heads))
    attended = heads_out.transpose(1, 0, 2).reshape(key_total, HEAD_TOTAL * HEAD_DIM).astype(jnp.bfloat16)
    mixed_sum = group_sum(attended, out_weight, HEAD_TOTAL // N_TP * HEAD_DIM)
    first_sum = residual.astype(jnp.float32) + rms_scale(mixed_sum, post_gain)
    ffn_in = rms_scale(first_sum, ffn_pre_gain).astype(jnp.bfloat16)
    gate_sum = jnp.dot(ffn_in, gate_weight, preferred_element_type=jnp.float32)
    up_sum = jnp.dot(ffn_in, up_weight, preferred_element_type=jnp.float32)
    hidden = (jax.nn.silu(gate_sum) * up_sum).astype(jnp.bfloat16)
    ffn_out = group_sum(hidden, down_weight, FF // N_TP)
    return (first_sum + 0.5 * rms_scale(ffn_out, ffn_post_gain)).astype(jnp.bfloat16)
```

```python
import functools

import jax
import jax.numpy as jnp
from jax import lax
from jax.experimental import pallas as pl
from jax.experimental.pallas import tpu as pltpu
from jax.sharding import PartitionSpec as P

HEAD_DIM = 64
norm_eps = 1e-06
MESH = pl.DeviceIdType.MESH
F32 = jnp.float32
BF16 = jnp.bfloat16


def rcopy(src, dst, send_sem, recv_sem, device):
    return pltpu.make_async_remote_copy(
        src_ref=src, dst_ref=dst, send_sem=send_sem, recv_sem=recv_sem,
        device_id=device, device_id_type=MESH,
    )


def layer_kernel(
    n, m,
    q_ref, k_ref, v_ref, res_ref, wo_ref, pg_ref, gate_ref, up_ref, down_ref, prg_ref, fg_ref,
    out_ref,
    kall, vall, gall, uall, dall, qm, tri, acc, acc_low, lost, att, sbuf, rbuf, res_v, first, x_all, hidden,
    fbuf, rb, ff,
    ring_send, ring_recv, rs_send, rs_recv, ag_send, ag_recv, fs_send, fs_recv, res_sem,
):
    s = lax.axis_index("sp")
    me = lax.axis_index("tp")
    nxt, prv = lax.rem(s + 1, n), lax.rem(s + n - 1, n)
    toks, width = q_ref.shape
    heads = width // HEAD_DIM
    d_rows = gate_ref.shape[0]
    f_half = down_ref.shape[0] // 2
    cols = down_ref.shape[1]
    d_model = wo_ref.shape[1]
    part = toks // m
    kc = min(256, toks)
    qt = min(128, toks)
    near, far = n // 2 - 1, n // 2

    barrier = pltpu.get_barrier_semaphore()
    for z in (nxt, prv):
        pl.semaphore_signal(barrier, inc=1, device_id={"sp": z}, device_id_type=MESH)
    for d in range(1, m):
        pl.semaphore_signal(barrier, inc=1, device_id={"tp": lax.rem(me + d, m)}, device_id_type=MESH)
    pl.semaphore_wait(barrier, m + 1)

    streams = [
        (k_ref, lambda o: kall.at[o], (far, near)),
        (v_ref, lambda o: vall.at[o], (far, near)),
        (gate_ref, lambda o: gall.at[pl.ds(pl.multiple_of(o * d_rows, d_rows), d_rows), :], (near, far)),
        (up_ref, lambda o: uall.at[pl.ds(pl.multiple_of(o * d_rows, d_rows), d_rows), :], (near, far)),
        (down_ref.at[pl.ds(0, f_half), :], lambda o: dall.at[o, pl.ds(0, f_half), :], (far, near)),
        (down_ref.at[pl.ds(f_half, f_half), :], lambda o: dall.at[o, pl.ds(f_half, f_half), :], (far, near)),
    ]

    def origin_out(way, k):
        return lax.rem(s + n - k, n) if way == 0 else lax.rem(s + k, n)

    def origin_in(way, k):
        return lax.rem(s + n - 1 - k, n) if way == 0 else lax.rem(s + 1 + k, n)

    def out_copy(i, way, k):
        own, place, _ = streams[i]
        at = place(origin_out(way, k))
        src = own if isinstance(k, int) and k == 0 else at
        return rcopy(src, at, ring_send.at[i, way, k], ring_recv.at[i, way, k], {"sp": nxt if way == 0 else prv})

    def in_copy(i, way, k):
        at = streams[i][1](origin_in(way, k))
        return rcopy(at, at, ring_send.at[i, way, k], ring_recv.at[i, way, k], {"sp": prv if way == 0 else nxt})

    def start_group(group):
        for i in group:
            for way in (0, 1):
                if streams[i][2][way]:
                    out_copy(i, way, 0).start()

    def service(group, k):
        for i in group:
            for way in (0, 1):
                hops = streams[i][2][way]
                if k < hops:
                    in_copy(i, way, k).wait_recv()
                    if k + 1 < hops:
                        out_copy(i, way, k + 1).start()

    def drain(group):
        for i in group:
            for way in (0, 1):
                for k in range(streams[i][2][way]):
                    out_copy(i, way, k).wait_send()

    KV, GU, DN = (0, 1), (2, 3), (4, 5)

    @pl.when(s < n - 1)
    def _():
        for i in KV:
            out_copy(i, 0, 0).start()

    @pl.when(s < near)
    def _():
        for i in KV:
            out_copy(i, 1, 0).start()

    res_copy = pltpu.make_async_copy(res_ref.at[pl.ds(pl.multiple_of(me * part, part), part), :], res_v, res_sem)
    res_copy.start()

    lane_head = lax.broadcasted_iota(jnp.int32, (toks, width), 1) // HEAD_DIM
    scaled = q_ref[...].astype(F32) * (1.0 / HEAD_DIM**0.5)
    for h in range(heads):
        qm[h] = jnp.where(lane_head == h, scaled, 0.0).astype(BF16)
    tri[...] = jnp.where(
        lax.broadcasted_iota(jnp.int32, (kc, kc), 0) > lax.broadcasted_iota(jnp.int32, (kc, kc), 1), 1.0, 0.0
    ).astype(BF16)
    acc_low[...] = jnp.zeros_like(acc_low)
    gall[pl.ds(pl.multiple_of(s * d_rows, d_rows), d_rows), :] = gate_ref[...]
    uall[pl.ds(pl.multiple_of(s * d_rows, d_rows), d_rows), :] = up_ref[...]

    def attend(keys, vals, mode):
        def tile(i, carry_in):
            rows = pl.ds(pl.multiple_of(i * qt, qt), qt)
            for h in range(heads):
                qtile = qm[h, rows, :]
                gone = lost[h, rows, :] if mode == "high" else jnp.zeros((qt, 1), F32)
                out = jnp.zeros((qt, width), F32)
                for c in reversed(range(toks // kc)):
                    z = lax.dot_general(
                        qtile, keys[pl.ds(c * kc, kc), :], (((1,), (1,)), ((), ())), preferred_element_type=F32
                    )
                    soft = jnp.maximum(z, 0.0) + jnp.log(1.0 + jnp.exp(-jnp.abs(z)))
                    take = z - soft
                    if mode == "own":
                        key_pos = c * kc + lax.broadcasted_iota(jnp.int32, (qt, kc), 1)
                        strict = key_pos < i * qt + lax.broadcasted_iota(jnp.int32, (qt, kc), 0)
                        soft = jnp.where(strict, soft, 0.0)
                    head = soft.astype(BF16)
                    rest = (soft - head.astype(F32)).astype(BF16)
                    later = jnp.dot(head, tri[...], preferred_element_type=F32) + jnp.dot(
                        rest, tri[...], preferred_element_type=F32
                    )
                    weight = jnp.exp(take - later - gone)
                    if mode == "own":
                        weight = jnp.where(strict, weight, 0.0)
                    out = out + jnp.dot(
                        weight.astype(BF16), vals[pl.ds(c * kc, kc), :], preferred_element_type=F32
                    )
                    gone = gone + later[:, 0:1] + soft[:, 0:1]
                if mode == "own":
                    acc[h, rows, :] = out
                    lost[h, rows, :] = gone
                elif mode == "high":
                    acc[h, rows, :] = acc[h, rows, :] + out
                    lost[h, rows, :] = gone
                else:
                    acc_low[h, rows, :] = acc_low[h, rows, :] * jnp.exp(-gone) + out
            return carry_in

        lax.fori_loop(0, toks // qt, tile, 0)

    attend(k_ref, v_ref, "own")

    def kv_step(k, carry_in):
        up_need = s - 1 - k >= 0
        wrap = lax.rem(s + 1 + k, n)
        down_need = jnp.logical_and(k < near, wrap < near)
        for i in KV:
            @pl.when(up_need)
            def _():
                in_copy(i, 0, k).wait_recv()

                @pl.when(jnp.logical_and(k + 1 < far, s < n - 1))
                def _():
                    out_copy(i, 0, k + 1).start()

            @pl.when(down_need)
            def _():
                in_copy(i, 1, k).wait_recv()

                @pl.when(k + 1 < near)
                def _():
                    out_copy(i, 1, k + 1).start()

        @pl.when(k == far - 2)
        def _():
            start_group(GU)

        @pl.when(up_need)
        def _():
            o = origin_in(0, k)
            attend(kall.at[o], vall.at[o], "high")

        @pl.when(jnp.logical_and(down_need, wrap < s))
        def _():
            attend(kall.at[wrap], vall.at[wrap], "low")

        return carry_in

    lax.fori_loop(0, far, kv_step, 0)

    whole = [acc[h] + acc_low[h] * jnp.exp(-lost[h]) for h in range(heads)]
    joined = whole[0]
    for h in range(1, heads):
        joined = jnp.where(lane_head == h, whole[h], joined)
    att[...] = joined.astype(BF16)
    nc = min(512, d_model)
    for c in range(d_model // nc):
        sbuf[:, pl.ds(c * nc, nc)] = jnp.dot(
            att[...], wo_ref[:, pl.ds(c * nc, nc)], preferred_element_type=F32
        ).astype(BF16)

    def rs_copy(d):
        p = lax.rem(me + d, m)
        return rcopy(
            sbuf.at[pl.ds(pl.multiple_of(p * part, part), part), :], rbuf.at[d - 1],
            rs_send.at[d - 1], rs_recv.at[d - 1], {"tp": p},
        )

    def ag_copy(d):
        mine = x_all.at[pl.ds(pl.multiple_of(me * part, part), part), :]
        return rcopy(mine, mine, ag_send.at[d - 1], ag_recv.at[d - 1], {"tp": lax.rem(me + d, m)})

    def ag_in(d):
        p = lax.rem(me + m - d, m)
        at = x_all.at[pl.ds(pl.multiple_of(p * part, part), part), :]
        return rcopy(at, at, ag_send.at[d - 1], ag_recv.at[d - 1], {"tp": p})

    for d in range(1, m):
        rs_copy(d).start()

    def norm(v, gain):
        mean_square = jnp.mean(v * v, axis=-1, keepdims=True)
        return v * lax.rsqrt(mean_square + norm_eps) * gain

    third = (far + 1) // 3
    for k in range(third):
        service(GU, k)
    for d in range(1, m):
        rs_copy(d).wait()
    mixed = sbuf[pl.ds(pl.multiple_of(me * part, part), part), :].astype(F32)
    for d in range(1, m):
        mixed = mixed + rbuf[d - 1].astype(F32)
    res_copy.wait()
    first[...] = res_v[...].astype(F32) + norm(mixed, pg_ref[...])
    x_all[pl.ds(pl.multiple_of(me * part, part), part), :] = norm(first[...], prg_ref[...]).astype(BF16)
    for d in range(1, m):
        ag_copy(d).start()
    for k in range(third, far):
        if k == far - 1:
            start_group(DN)
        service(GU, k)
    for d in range(1, m):
        ag_in(d).wait_recv()

    mt = min(256, toks)

    def ffn_tile(i, carry_in):
        rows = pl.ds(pl.multiple_of(i * mt, mt), mt)
        g = jnp.dot(x_all[rows, :], gall[...], preferred_element_type=F32)
        u = jnp.dot(x_all[rows, :], uall[...], preferred_element_type=F32)
        hidden[rows, :] = (g / (1.0 + jnp.exp(-g)) * u).astype(BF16)
        return carry_in

    lax.fori_loop(0, toks // mt, ffn_tile, 0)

    def fs_copy(c, wide, d):
        p = lax.rem(me + d, m)
        return rcopy(
            fbuf.at[c, pl.ds(pl.multiple_of(p * part, part), part), pl.ds(0, wide)], rb.at[c, d - 1, :, pl.ds(0, wide)],
            fs_send.at[c, d - 1], fs_recv.at[c, d - 1], {"tp": p},
        )

    def chunk_origins(c):
        if c == 0:
            return [s]
        return [origin_in(way, c - 1) for way in (0, 1) if c - 1 < streams[DN[0]][2][way]]

    for c in range(far + 1):
        if c:
            service(DN, c - 1)
        origins = chunk_origins(c)
        tiles = [down_ref[...] if c == 0 else dall[o] for o in origins]
        wide = cols * len(tiles)
        both = tiles[0] if len(tiles) == 1 else jnp.concatenate(tiles, axis=1)
        fbuf[c, :, pl.ds(0, wide)] = jnp.dot(hidden[...], both, preferred_element_type=F32).astype(BF16)
        for d in range(1, m):
            fs_copy(c, wide, d).start()

    square = jnp.zeros((part, 1), F32)
    for c in range(far + 1):
        origins = chunk_origins(c)
        wide = cols * len(origins)
        for d in range(1, m):
            fs_copy(c, wide, d).wait()
        total = fbuf[c, pl.ds(pl.multiple_of(me * part, part), part), pl.ds(0, wide)].astype(F32)
        for d in range(1, m):
            total = total + rb[c, d - 1, :, pl.ds(0, wide)].astype(F32)
        square = square + jnp.sum(total * total, axis=-1, keepdims=True)
        for j, o in enumerate(origins):
            ff[o] = total[:, j * cols : (j + 1) * cols]
    scale = lax.rsqrt(square / d_model + norm_eps)
    for o in range(n):
        at = pl.ds(o * cols, cols)
        out_ref[:, at] = (first[:, at] + 0.5 * (ff[o] * scale * fg_ref[:, at])).astype(out_ref.dtype)

    for d in range(1, m):
        ag_copy(d).wait_send()

    def kv_drain(k, carry_in):
        for i in KV:
            @pl.when(jnp.logical_and(s < n - 1, s - k >= 0))
            def _():
                out_copy(i, 0, k).wait_send()

            @pl.when(jnp.logical_and(k < near, lax.rem(s + k, n) < near))
            def _():
                out_copy(i, 1, k).wait_send()

        return carry_in

    lax.fori_loop(0, far, kv_drain, 0)
    drain(GU)
    drain(DN)


def solution(mesh):
    n, m = mesh.shape["sp"], mesh.shape["tp"]

    def per_device(q, k, v, residual, wo, pg, gate, up, down, prg, fg):
        toks, width = q.shape
        d_model = wo.shape[1]
        f_loc = gate.shape[1]
        heads = width // HEAD_DIM
        part = toks // m
        cols = down.shape[1]
        far = n // 2
        chunks = far + 1
        kc = min(256, toks)
        vm, dma = pltpu.VMEM, pltpu.SemaphoreType.DMA
        in_vmem = pl.BlockSpec(memory_space=vm)
        specs = [in_vmem] * 11
        specs[3] = pl.BlockSpec(memory_space=pl.ANY)
        flops = 2 * toks * (n * toks * width * 4 + width * d_model + 3 * d_model * f_loc)
        return pl.pallas_call(
            functools.partial(layer_kernel, n, m),
            out_shape=jax.ShapeDtypeStruct((part, d_model), BF16),
            in_specs=specs,
            out_specs=in_vmem,
            scratch_shapes=[
                vm((n, toks, width), BF16),
                vm((n, toks, width), BF16),
                vm((d_model, f_loc), BF16),
                vm((d_model, f_loc), BF16),
                vm((n, f_loc, cols), BF16),
                vm((heads, toks, width), BF16),
                vm((kc, kc), BF16),
                vm((heads, toks, width), F32),
                vm((heads, toks, width), F32),
                vm((heads, toks, 1), F32),
                vm((toks, width), BF16),
                vm((toks, d_model), BF16),
                vm((m - 1, part, d_model), BF16),
                vm((part, d_model), BF16),
                vm((part, d_model), F32),
                vm((toks, d_model), BF16),
                vm((toks, f_loc), BF16),
                vm((chunks, toks, 2 * cols), BF16),
                vm((chunks, m - 1, part, 2 * cols), BF16),
                vm((n, part, cols), F32),
                dma((6, 2, far)),
                dma((6, 2, far)),
                dma((m - 1,)),
                dma((m - 1,)),
                dma((m - 1,)),
                dma((m - 1,)),
                dma((chunks, m - 1)),
                dma((chunks, m - 1)),
                dma,
            ],
            compiler_params=pltpu.CompilerParams(
                collective_id=0, has_side_effects=True, vmem_limit_bytes=60 * 1024 * 1024
            ),
            cost_estimate=pl.CostEstimate(flops=flops, bytes_accessed=4 * toks * d_model, transcendentals=0),
        )(q, k, v, residual, wo, pg.reshape(1, -1), gate, up, down, prg.reshape(1, -1), fg.reshape(1, -1))

    in_specs = (
        P(("grp", "sp"), "tp"),
        P(("grp", "sp"), "tp"),
        P(("grp", "sp"), "tp"),
        P(("grp", "sp"), None),
        P("tp", None),
        P(),
        P("sp", "tp"),
        P("sp", "tp"),
        P("tp", "sp"),
        P(),
        P(),
    )
    out_specs = P(("grp", "sp", "tp"), None)
    return jax.shard_map(per_device, mesh=mesh, in_specs=in_specs, out_specs=out_specs, check_vma=False)
```

```python
import functools

import jax
import jax.numpy as jnp
from jax import lax
from jax.experimental import pallas as pl
from jax.experimental.pallas import tpu as pltpu
from jax.sharding import PartitionSpec as P

HEAD_DIM = 64
norm_eps = 1e-06
LOG2_E = 1.4426950408889634
MESH = pl.DeviceIdType.MESH
F32 = jnp.float32
BF16 = jnp.bfloat16


def rcopy(src, dst, send_sem, recv_sem, device):
    return pltpu.make_async_remote_copy(
        src_ref=src, dst_ref=dst, send_sem=send_sem, recv_sem=recv_sem,
        device_id=device, device_id_type=MESH,
    )


def layer_kernel(
    groups, n, m,
    q_ref, k_ref, v_ref, res_ref, wo_ref, pg_ref, gate_ref, up_ref, down_ref, prg_ref, fg_ref,
    out_ref,
    kall, vall, gall, uall, dall, qm, tri, acc, acc_low, lost, att, sbuf, pbuf, tbuf, hbuf, cbuf, res_v, first, x_all, hidden,
    fbuf, rb, ff,
    ring_send, ring_recv, cross_send, cross_recv, rs_send, rs_recv, ag_send, ag_recv, fs_send, fs_recv, res_sem,
):
    g = lax.axis_index("grp")
    s = lax.axis_index("sp")
    me = lax.axis_index("tp")
    nxt, prv = lax.rem(s + 1, n), lax.rem(s + n - 1, n)
    toks, width = q_ref.shape
    heads = width // HEAD_DIM
    d_rows = gate_ref.shape[0]
    f_half = down_ref.shape[0] // 2
    cols = down_ref.shape[1]
    d_model = wo_ref.shape[1]
    part = toks // m
    kc = min(256, toks)
    qt = min(256, toks)
    near, far = n // 2 - 1, n // 2

    barrier = pltpu.get_barrier_semaphore()
    for z in (nxt, prv):
        pl.semaphore_signal(barrier, inc=1, device_id={"sp": z}, device_id_type=MESH)
    for d in range(1, m):
        pl.semaphore_signal(barrier, inc=1, device_id={"tp": lax.rem(me + d, m)}, device_id_type=MESH)
    sides = sorted({1 % groups, groups - 1} - {0})
    for d in sides:
        pl.semaphore_signal(barrier, inc=1, device_id={"grp": lax.rem(g + d, groups)}, device_id_type=MESH)
    pl.semaphore_wait(barrier, m + 1 + len(sides))

    d_half = d_rows // 2

    def w_rows(ref, begin, size):
        return lambda o: ref.at[pl.ds(pl.multiple_of(o * d_rows + begin, size), size), :]

    streams = [
        (k_ref, lambda o: kall.at[o], (far, near), False),
        (v_ref, lambda o: vall.at[o], (far, near), False),
        (gate_ref, w_rows(gall, 0, d_rows), (near, far), True),
        (up_ref.at[pl.ds(0, d_half), :], w_rows(uall, 0, d_half), (near, far), False),
        (up_ref.at[pl.ds(d_half, d_half), :], w_rows(uall, d_half, d_half), (near, far), True),
        (down_ref.at[pl.ds(0, f_half), :], lambda o: dall.at[o, pl.ds(0, f_half), :], (far, near), False),
        (down_ref.at[pl.ds(f_half, f_half), :], lambda o: dall.at[o, pl.ds(f_half, f_half), :], (far, near), False),
    ]
    split = [i for i, stream in enumerate(streams) if stream[3]]
    cross_hops = (groups // 2, groups - 1 - groups // 2)
    shares = n // groups

    def carried(i, o, act):
        if streams[i][3] and groups > 1:
            pl.when(lax.rem(o, groups) == g)(act)
        else:
            act()

    def cross_copy(i, o, way, k):
        at, j = streams[i][1](o), split.index(i)
        side = lax.rem(g + (1 if way == 0 else groups - 1), groups)
        sems = (j, o // groups, way, k)
        return rcopy(at, at, cross_send.at[sems], cross_recv.at[sems], {"grp": side})

    def cross_class(way, k, incoming):
        hop = k + incoming
        return lax.rem(g + groups - hop, groups) if way == 0 else lax.rem(g + hop, groups)

    def cross_each(i, k, incoming, act):
        for way in (0, 1):
            if k < cross_hops[way]:
                for b in range(shares):
                    o = b * groups + cross_class(way, k, incoming)
                    pl.when(o != s)(functools.partial(act, i, o, way, k))

    def cross_step(k):
        def take(i, o, way, k):
            cross_copy(i, o, way, k).wait_recv()
            if k + 1 < cross_hops[way]:
                cross_copy(i, o, way, k + 1).start()

        for i in split:
            cross_each(i, k, 1, take)

    def cross_drain():
        for i in split:
            for k in range(cross_hops[0]):
                cross_each(i, k, 0, lambda i, o, way, k: cross_copy(i, o, way, k).wait_send())

    def origin_out(way, k):
        return lax.rem(s + n - k, n) if way == 0 else lax.rem(s + k, n)

    def origin_in(way, k):
        return lax.rem(s + n - 1 - k, n) if way == 0 else lax.rem(s + 1 + k, n)

    def out_copy(i, way, k):
        own, place = streams[i][:2]
        at = place(origin_out(way, k))
        src = own if isinstance(k, int) and k == 0 else at
        return rcopy(src, at, ring_send.at[i, way, k], ring_recv.at[i, way, k], {"sp": nxt if way == 0 else prv})

    def in_copy(i, way, k):
        at = streams[i][1](origin_in(way, k))
        return rcopy(at, at, ring_send.at[i, way, k], ring_recv.at[i, way, k], {"sp": prv if way == 0 else nxt})

    def start_group(group):
        for i in group:
            for way in (0, 1):
                if streams[i][2][way]:
                    carried(i, s, out_copy(i, way, 0).start)

    def service(group, k):
        for i in group:
            for way in (0, 1):
                hops = streams[i][2][way]
                if k < hops:
                    o = origin_in(way, k)

                    def pass_on(i=i, way=way, hops=hops, o=o):
                        in_copy(i, way, k).wait_recv()
                        if k + 1 < hops:
                            out_copy(i, way, k + 1).start()
                        if streams[i][3]:
                            for across in (0, 1):
                                if cross_hops[across]:
                                    cross_copy(i, o, across, 0).start()

                    carried(i, o, pass_on)

    def drain(group):
        for i in group:
            for way in (0, 1):
                for k in range(streams[i][2][way]):
                    carried(i, origin_out(way, k), out_copy(i, way, k).wait_send)

    KV, GU, DN = (0, 1), (2, 3, 4), (5, 6)

    @pl.when(s < n - 1)
    def _():
        for i in KV:
            out_copy(i, 0, 0).start()

    @pl.when(s < near)
    def _():
        for i in KV:
            out_copy(i, 1, 0).start()

    res_copy = pltpu.make_async_copy(res_ref.at[pl.ds(pl.multiple_of(me * part, part), part), :], res_v, res_sem)
    res_copy.start()

    lane_head = lax.broadcasted_iota(jnp.int32, (toks, width), 1) // HEAD_DIM
    scaled = q_ref[...].astype(F32) * (1.0 / HEAD_DIM**0.5)
    for h in range(heads):
        qm[h] = jnp.where(lane_head == h, scaled, 0.0).astype(BF16)
    tri[...] = jnp.where(
        lax.broadcasted_iota(jnp.int32, (kc, kc), 0) > lax.broadcasted_iota(jnp.int32, (kc, kc), 1), 1.0, 0.0
    ).astype(BF16)
    acc_low[...] = jnp.zeros_like(acc_low)
    gall[pl.ds(pl.multiple_of(s * d_rows, d_rows), d_rows), :] = gate_ref[...]
    uall[pl.ds(pl.multiple_of(s * d_rows, d_rows), d_rows), :] = up_ref[...]

    def attend(keys, vals, mode):
        def tile(i, carry_in):
            rows = pl.ds(pl.multiple_of(i * qt, qt), qt)
            for h in range(heads):
                qtile = qm[h, rows, :]
                gone = lost[h, rows, :] if mode == "high" else jnp.zeros((qt, 1), F32)
                out = jnp.zeros((qt, width), F32)
                for c in reversed(range(toks // kc)):
                    z = lax.dot_general(
                        qtile, keys[pl.ds(c * kc, kc), :], (((1,), (1,)), ((), ())), preferred_element_type=F32
                    )
                    soft = jnp.maximum(z, 0.0) + jnp.log(1.0 + jnp.exp2(jnp.abs(z) * -LOG2_E))
                    take = z - soft
                    if mode == "own":
                        key_pos = c * kc + lax.broadcasted_iota(jnp.int32, (qt, kc), 1)
                        strict = key_pos < i * qt + lax.broadcasted_iota(jnp.int32, (qt, kc), 0)
                        soft = jnp.where(strict, soft, 0.0)
                    head = soft.astype(BF16)
                    rest = (soft - head.astype(F32)).astype(BF16)
                    later = jnp.dot(head, tri[...], preferred_element_type=F32) + jnp.dot(
                        rest, tri[...], preferred_element_type=F32
                    )
                    weight = jnp.exp(take - later - gone)
                    if mode == "own":
                        weight = jnp.where(strict, weight, 0.0)
                    out = out + jnp.dot(
                        weight.astype(BF16), vals[pl.ds(c * kc, kc), :], preferred_element_type=F32
                    )
                    gone = gone + later[:, 0:1] + soft[:, 0:1]
                if mode == "own":
                    acc[h, rows, :] = out
                    lost[h, rows, :] = gone
                elif mode == "high":
                    acc[h, rows, :] = acc[h, rows, :] + out
                    lost[h, rows, :] = gone
                else:
                    acc_low[h, rows, :] = acc_low[h, rows, :] * jnp.exp(-gone) + out
            return carry_in

        lax.fori_loop(0, toks // qt, tile, 0)

    attend(k_ref, v_ref, "own")

    def kv_step(k, carry_in):
        up_need = s - 1 - k >= 0
        wrap = lax.rem(s + 1 + k, n)
        down_need = jnp.logical_and(k < near, wrap < near)
        for i in KV:
            @pl.when(up_need)
            def _():
                in_copy(i, 0, k).wait_recv()

                @pl.when(jnp.logical_and(k + 1 < far, s < n - 1))
                def _():
                    out_copy(i, 0, k + 1).start()

            @pl.when(down_need)
            def _():
                in_copy(i, 1, k).wait_recv()

                @pl.when(k + 1 < near)
                def _():
                    out_copy(i, 1, k + 1).start()

        @pl.when(k == far - 2)
        def _():
            start_group(GU)

        @pl.when(k == far - 1)
        def _():
            service(GU, 0)

        @pl.when(up_need)
        def _():
            o = origin_in(0, k)
            attend(kall.at[o], vall.at[o], "high")

        @pl.when(jnp.logical_and(down_need, wrap < s))
        def _():
            attend(kall.at[wrap], vall.at[wrap], "low")

        return carry_in

    lax.fori_loop(0, far, kv_step, 0)

    whole = [acc[h] + acc_low[h] * jnp.exp(-lost[h]) for h in range(heads)]
    joined = whole[0]
    for h in range(1, heads):
        joined = jnp.where(lane_head == h, whole[h], joined)
    att[...] = joined.astype(BF16)
    nc = min(512, d_model)
    for c in range(d_model // nc):
        sbuf[:, pl.ds(c * nc, nc)] = jnp.dot(
            att[...], wo_ref[:, pl.ds(c * nc, nc)], preferred_element_type=F32
        ).astype(BF16)

    n_x = m // 2
    assert n_x == 4
    x, core = me // 2, lax.rem(me, 2)
    x_up, x_far, x_dn = lax.rem(x + 1, n_x), lax.rem(x + 2, n_x), lax.rem(x + 3, n_x)
    mate = {"tp": 2 * x + 1 - core}
    up_dev, dn_dev = {"tp": 2 * x_up + core}, {"tp": 2 * x_dn + core}
    hp = part // 2
    top, bottom = pl.ds(0, hp), pl.ds(hp, hp)

    def rows_of(at_x, at_core, begin=0, size=part):
        return pl.ds(pl.multiple_of((2 * at_x + at_core) * part + begin, size), size)

    order = (x_far, x_up, x_dn, x)

    def pair_copy(j):
        return rcopy(sbuf.at[rows_of(order[j], 1 - core), :], pbuf.at[j], rs_send.at[j], rs_recv.at[j], mate)

    far_up = rcopy(tbuf.at[0, top, :], hbuf.at[0], rs_send.at[4], rs_recv.at[4], up_dev)
    far_dn = rcopy(tbuf.at[0, bottom, :], hbuf.at[1], rs_send.at[5], rs_recv.at[5], dn_dev)
    raw_up = rcopy(tbuf.at[1, bottom, :], hbuf.at[2], rs_send.at[6], rs_recv.at[6], up_dev)
    raw_dn = rcopy(tbuf.at[2, top, :], hbuf.at[3], rs_send.at[7], rs_recv.at[7], dn_dev)
    sum_up = rcopy(cbuf.at[0], hbuf.at[4], rs_send.at[8], rs_recv.at[8], up_dev)
    sum_dn = rcopy(cbuf.at[1], hbuf.at[5], rs_send.at[9], rs_recv.at[9], dn_dev)
    rs_along = (far_up, far_dn, raw_up, raw_dn, sum_up, sum_dn)

    def ag_to(i, at_x, device, begin=0, size=part):
        at = x_all.at[rows_of(at_x, core, begin, size), :]
        return rcopy(at, at, ag_send.at[i], ag_recv.at[i], device)

    def ag_from(i, at_x, at_core, begin=0, size=part):
        at = x_all.at[rows_of(at_x, at_core, begin, size), :]
        return rcopy(at, at, ag_send.at[i], ag_recv.at[i], mate)

    ag_out = [
        ag_to(0, x, up_dev), ag_to(1, x, dn_dev), ag_to(2, x, mate),
        ag_to(3, x_dn, up_dev, 0, hp), ag_to(4, x_dn, mate),
        ag_to(5, x_up, dn_dev, hp, hp), ag_to(6, x_up, mate),
        ag_to(7, x_far, mate, 0, hp), ag_to(8, x_far, mate, hp, hp),
    ]
    ag_in = [
        ag_from(0, x_dn, core), ag_from(1, x_up, core), ag_from(2, x, 1 - core),
        ag_from(3, x_far, core, 0, hp), ag_from(4, x_dn, 1 - core),
        ag_from(5, x_far, core, hp, hp), ag_from(6, x_up, 1 - core),
        ag_from(7, x_far, 1 - core, 0, hp), ag_from(8, x_far, 1 - core, hp, hp),
    ]

    def norm(v, gain):
        mean_square = jnp.mean(v * v, axis=-1, keepdims=True)
        return v * lax.rsqrt(mean_square + norm_eps) * gain

    def ring_step(j):
        if j < far:
            service(GU, j)

    for j in range(4):
        pair_copy(j).start()
    ring_step(1)
    for j in range(4):
        pair_copy(j).wait_recv()
        pair = sbuf[rows_of(order[j], core), :].astype(F32) + pbuf[j].astype(F32)
        if j == 3:
            first[...] = pair
        else:
            tbuf[j] = pair.astype(BF16)
            for copy in ((far_up, far_dn), (raw_up,), (raw_dn,))[j]:
                copy.start()
    ring_step(2)
    far_up.wait_recv()
    cbuf[0] = (tbuf[1, top, :].astype(F32) + hbuf[0].astype(F32)).astype(BF16)
    sum_up.start()
    far_dn.wait_recv()
    cbuf[1] = (tbuf[2, bottom, :].astype(F32) + hbuf[1].astype(F32)).astype(BF16)
    sum_dn.start()
    ring_step(3)
    res_copy.wait()
    for copy in (raw_up, raw_dn, sum_up, sum_dn):
        copy.wait_recv()
    for half, (raw, summed) in ((top, (3, 4)), (bottom, (2, 5))):
        mixed = first[half, :] + hbuf[raw].astype(F32) + hbuf[summed].astype(F32)
        first[half, :] = res_v[half, :].astype(F32) + norm(mixed, pg_ref[...])
    x_all[rows_of(x, core), :] = norm(first[...], prg_ref[...]).astype(BF16)
    for i in (0, 1, 2):
        ag_out[i].start()
    ring_step(4)
    ag_in[0].wait_recv()
    for i in (3, 4):
        ag_out[i].start()
    ag_in[1].wait_recv()
    for i in (5, 6):
        ag_out[i].start()
    ring_step(5)
    ag_in[3].wait_recv()
    ag_out[7].start()
    ag_in[5].wait_recv()
    ag_out[8].start()
    start_group(DN)
    for k in range(6, far):
        ring_step(k)
    early = min(far, max(1, cross_hops[0] - 1))
    for k in range(max(early, cross_hops[0])):
        if k < early:
            service(DN, k)
        if k < cross_hops[0]:
            cross_step(k)
    for i in (2, 4, 6, 7, 8):
        ag_in[i].wait_recv()

    mt = min(256, toks)

    def ffn_tile(i, carry_in):
        rows = pl.ds(pl.multiple_of(i * mt, mt), mt)
        g = jnp.dot(x_all[rows, :], gall[...], preferred_element_type=F32)
        u = jnp.dot(x_all[rows, :], uall[...], preferred_element_type=F32)
        hidden[rows, :] = (g / (1.0 + jnp.exp(-g)) * u).astype(BF16)
        return carry_in

    lax.fori_loop(0, toks // mt, ffn_tile, 0)

    def fs_copy(c, wide, d):
        p = lax.rem(me + d, m)
        return rcopy(
            fbuf.at[c, pl.ds(pl.multiple_of(p * part, part), part), pl.ds(0, wide)], rb.at[c, d - 1, :, pl.ds(0, wide)],
            fs_send.at[c, d - 1], fs_recv.at[c, d - 1], {"tp": p},
        )

    def chunk_origins(c):
        if c == 0:
            return [s]
        return [origin_in(way, c - 1) for way in (0, 1) if c - 1 < streams[DN[0]][2][way]]

    def finish(c, square):
        origins = chunk_origins(c)
        wide = cols * len(origins)
        for d in range(1, m):
            fs_copy(c, wide, d).wait()
        total = fbuf[c, pl.ds(pl.multiple_of(me * part, part), part), pl.ds(0, wide)].astype(F32)
        for d in range(1, m):
            total = total + rb[c, d - 1, :, pl.ds(0, wide)].astype(F32)
        for j, o in enumerate(origins):
            ff[o] = total[:, j * cols : (j + 1) * cols]
        return square + jnp.sum(total * total, axis=-1, keepdims=True)

    square = jnp.zeros((part, 1), F32)
    behind = 3
    for c in range(far + 1):
        if c > early:
            service(DN, c - 1)
        origins = chunk_origins(c)
        tiles = [down_ref[...] if c == 0 else dall[o] for o in origins]
        wide = cols * len(tiles)
        both = tiles[0] if len(tiles) == 1 else jnp.concatenate(tiles, axis=1)
        fbuf[c, :, pl.ds(0, wide)] = jnp.dot(hidden[...], both, preferred_element_type=F32).astype(BF16)
        for d in range(1, m):
            fs_copy(c, wide, d).start()
        if c >= behind:
            square = finish(c - behind, square)
    for c in range(max(0, far + 1 - behind), far + 1):
        square = finish(c, square)
    scale = lax.rsqrt(square / d_model + norm_eps)
    for o in range(n):
        at = pl.ds(o * cols, cols)
        out_ref[:, at] = (first[:, at] + 0.5 * (ff[o] * scale * fg_ref[:, at])).astype(out_ref.dtype)

    for j in range(4):
        pair_copy(j).wait_send()
    for copy in rs_along:
        copy.wait_send()
    for copy in ag_out:
        copy.wait_send()

    def kv_drain(k, carry_in):
        for i in KV:
            @pl.when(jnp.logical_and(s < n - 1, s - k >= 0))
            def _():
                out_copy(i, 0, k).wait_send()

            @pl.when(jnp.logical_and(k < near, lax.rem(s + k, n) < near))
            def _():
                out_copy(i, 1, k).wait_send()

        return carry_in

    lax.fori_loop(0, far, kv_drain, 0)
    drain(GU)
    cross_drain()
    drain(DN)


def solution(mesh):
    groups, n, m = mesh.shape["grp"], mesh.shape["sp"], mesh.shape["tp"]

    def per_device(q, k, v, residual, wo, pg, gate, up, down, prg, fg):
        toks, width = q.shape
        d_model = wo.shape[1]
        f_loc = gate.shape[1]
        heads = width // HEAD_DIM
        part = toks // m
        cols = down.shape[1]
        far = n // 2
        chunks = far + 1
        kc = min(256, toks)
        vm, dma = pltpu.VMEM, pltpu.SemaphoreType.DMA
        in_vmem = pl.BlockSpec(memory_space=vm)
        specs = [in_vmem] * 11
        specs[3] = pl.BlockSpec(memory_space=pl.ANY)
        flops = 2 * toks * (n * toks * width * 4 + width * d_model + 3 * d_model * f_loc)
        return pl.pallas_call(
            functools.partial(layer_kernel, groups, n, m),
            out_shape=jax.ShapeDtypeStruct((part, d_model), BF16),
            in_specs=specs,
            out_specs=in_vmem,
            scratch_shapes=[
                vm((n, toks, width), BF16),
                vm((n, toks, width), BF16),
                vm((d_model, f_loc), BF16),
                vm((d_model, f_loc), BF16),
                vm((n, f_loc, cols), BF16),
                vm((heads, toks, width), BF16),
                vm((kc, kc), BF16),
                vm((heads, toks, width), F32),
                vm((heads, toks, width), F32),
                vm((heads, toks, 1), F32),
                vm((toks, width), BF16),
                vm((toks, d_model), BF16),
                vm((4, part, d_model), BF16),
                vm((3, part, d_model), BF16),
                vm((6, part // 2, d_model), BF16),
                vm((2, part // 2, d_model), BF16),
                vm((part, d_model), BF16),
                vm((part, d_model), F32),
                vm((toks, d_model), BF16),
                vm((toks, f_loc), BF16),
                vm((chunks, toks, 2 * cols), BF16),
                vm((chunks, m - 1, part, 2 * cols), BF16),
                vm((n, part, cols), F32),
                dma((7, 2, far)),
                dma((7, 2, far)),
                dma((2, n // groups, 2, max(1, groups // 2))),
                dma((2, n // groups, 2, max(1, groups // 2))),
                dma((10,)),
                dma((10,)),
                dma((9,)),
                dma((9,)),
                dma((chunks, m - 1)),
                dma((chunks, m - 1)),
                dma,
            ],
            compiler_params=pltpu.CompilerParams(
                collective_id=0, has_side_effects=True, vmem_limit_bytes=60 * 1024 * 1024
            ),
            cost_estimate=pl.CostEstimate(flops=flops, bytes_accessed=4 * toks * d_model, transcendentals=0),
        )(q, k, v, residual, wo, pg.reshape(1, -1), gate, up, down, prg.reshape(1, -1), fg.reshape(1, -1))

    in_specs = (
        P(("grp", "sp"), "tp"),
        P(("grp", "sp"), "tp"),
        P(("grp", "sp"), "tp"),
        P(("grp", "sp"), None),
        P("tp", None),
        P(),
        P("sp", "tp"),
        P("sp", "tp"),
        P("tp", "sp"),
        P(),
        P(),
    )
    out_specs = P(("grp", "sp", "tp"), None)
    return jax.shard_map(per_device, mesh=mesh, in_specs=in_specs, out_specs=out_specs, check_vma=False)
```

```python
import functools

import jax
import jax.numpy as jnp
from jax import lax
from jax.experimental import pallas as pl
from jax.experimental.pallas import tpu as pltpu
from jax.sharding import PartitionSpec as P

HEAD_DIM = 64
norm_eps = 1e-06
N_COL_GROUPS = 3
LOG2_E = 1.4426950408889634
MESH = pl.DeviceIdType.MESH
F32 = jnp.float32
BF16 = jnp.bfloat16


def rcopy(src, dst, send_sem, recv_sem, device):
    return pltpu.make_async_remote_copy(
        src_ref=src, dst_ref=dst, send_sem=send_sem, recv_sem=recv_sem,
        device_id=device, device_id_type=MESH,
    )


def layer_kernel(
    groups, n, m,
    q_ref, k_ref, v_ref, res_ref, wo_ref, pg_ref, gate_ref, up_ref, down_ref, prg_ref, fg_ref,
    out_ref,
    kall, vall, gall, uall, dall, qm, tri, acc, acc_low, lost, att, sbuf, pbuf, tbuf, hbuf, cbuf, res_v, first, x_all, hidden,
    fbuf, pb, tb, hb, cb, kept, ff,
    ring_send, ring_recv, cross_send, cross_recv, rs_send, rs_recv, ag_send, ag_recv, fs_send, fs_recv, res_sem,
):
    g = lax.axis_index("grp")
    s = lax.axis_index("sp")
    me = lax.axis_index("tp")
    nxt, prv = lax.rem(s + 1, n), lax.rem(s + n - 1, n)
    toks, width = q_ref.shape
    heads = width // HEAD_DIM
    d_rows = gate_ref.shape[0]
    f_half = down_ref.shape[0] // 2
    cols = down_ref.shape[1]
    d_model = wo_ref.shape[1]
    part = toks // m
    kc = min(256, toks)
    qt = min(512, toks)
    near, far = n // 2 - 1, n // 2

    barrier = pltpu.get_barrier_semaphore()
    for z in (nxt, prv):
        pl.semaphore_signal(barrier, inc=1, device_id={"sp": z}, device_id_type=MESH)
    for d in range(1, m):
        pl.semaphore_signal(barrier, inc=1, device_id={"tp": lax.rem(me + d, m)}, device_id_type=MESH)
    sides = sorted({1 % groups, groups - 1} - {0})
    for d in sides:
        pl.semaphore_signal(barrier, inc=1, device_id={"grp": lax.rem(g + d, groups)}, device_id_type=MESH)
    pl.semaphore_wait(barrier, m + 1 + len(sides))

    d_half = d_rows // 2

    def w_rows(ref, begin, size):
        return lambda o: ref.at[pl.ds(pl.multiple_of(o * d_rows + begin, size), size), :]

    streams = [
        (k_ref, lambda o: kall.at[o], (far, near), False),
        (v_ref, lambda o: vall.at[o], (far, near), False),
        (gate_ref, w_rows(gall, 0, d_rows), (near, far), True),
        (up_ref.at[pl.ds(0, d_half), :], w_rows(uall, 0, d_half), (near, far), False),
        (up_ref.at[pl.ds(d_half, d_half), :], w_rows(uall, d_half, d_half), (near, far), True),
        (down_ref.at[pl.ds(0, f_half), :], lambda o: dall.at[o, pl.ds(0, f_half), :], (far, near), False),
        (down_ref.at[pl.ds(f_half, f_half), :], lambda o: dall.at[o, pl.ds(f_half, f_half), :], (far, near), False),
    ]
    split = [i for i, stream in enumerate(streams) if stream[3]]
    cross_hops = (groups // 2, groups - 1 - groups // 2)
    shares = n // groups

    def carried(i, o, act):
        if streams[i][3] and groups > 1:
            pl.when(lax.rem(o, groups) == g)(act)
        else:
            act()

    def cross_copy(i, o, way, k):
        at, j = streams[i][1](o), split.index(i)
        side = lax.rem(g + (1 if way == 0 else groups - 1), groups)
        sems = (j, o // groups, way, k)
        return rcopy(at, at, cross_send.at[sems], cross_recv.at[sems], {"grp": side})

    def cross_class(way, k, incoming):
        hop = k + incoming
        return lax.rem(g + groups - hop, groups) if way == 0 else lax.rem(g + hop, groups)

    def cross_each(i, k, incoming, act):
        for way in (0, 1):
            if k < cross_hops[way]:
                for b in range(shares):
                    o = b * groups + cross_class(way, k, incoming)
                    pl.when(o != s)(functools.partial(act, i, o, way, k))

    def cross_step(k):
        def take(i, o, way, k):
            cross_copy(i, o, way, k).wait_recv()
            if k + 1 < cross_hops[way]:
                cross_copy(i, o, way, k + 1).start()

        for i in split:
            cross_each(i, k, 1, take)

    def cross_drain():
        for i in split:
            for k in range(cross_hops[0]):
                cross_each(i, k, 0, lambda i, o, way, k: cross_copy(i, o, way, k).wait_send())

    def origin_out(way, k):
        return lax.rem(s + n - k, n) if way == 0 else lax.rem(s + k, n)

    def origin_in(way, k):
        return lax.rem(s + n - 1 - k, n) if way == 0 else lax.rem(s + 1 + k, n)

    def out_copy(i, way, k):
        own, place = streams[i][:2]
        at = place(origin_out(way, k))
        src = own if isinstance(k, int) and k == 0 else at
        return rcopy(src, at, ring_send.at[i, way, k], ring_recv.at[i, way, k], {"sp": nxt if way == 0 else prv})

    def in_copy(i, way, k):
        at = streams[i][1](origin_in(way, k))
        return rcopy(at, at, ring_send.at[i, way, k], ring_recv.at[i, way, k], {"sp": prv if way == 0 else nxt})

    def start_group(group):
        for i in group:
            for way in (0, 1):
                if streams[i][2][way]:
                    carried(i, s, out_copy(i, way, 0).start)

    def service(group, k):
        for i in group:
            for way in (0, 1):
                hops = streams[i][2][way]
                if k < hops:
                    o = origin_in(way, k)

                    def pass_on(i=i, way=way, hops=hops, o=o):
                        in_copy(i, way, k).wait_recv()
                        if k + 1 < hops:
                            out_copy(i, way, k + 1).start()
                        if streams[i][3]:
                            for across in (0, 1):
                                if cross_hops[across]:
                                    cross_copy(i, o, across, 0).start()

                    carried(i, o, pass_on)

    def drain(group):
        for i in group:
            for way in (0, 1):
                for k in range(streams[i][2][way]):
                    carried(i, origin_out(way, k), out_copy(i, way, k).wait_send)

    KV, GU, DN = (0, 1), (2, 3, 4), (5, 6)

    @pl.when(s < n - 1)
    def _():
        for i in KV:
            out_copy(i, 0, 0).start()

    @pl.when(s < near)
    def _():
        for i in KV:
            out_copy(i, 1, 0).start()

    res_copy = pltpu.make_async_copy(res_ref.at[pl.ds(pl.multiple_of(me * part, part), part), :], res_v, res_sem)
    res_copy.start()

    lane_head = lax.broadcasted_iota(jnp.int32, (toks, width), 1) // HEAD_DIM
    scaled = q_ref[...].astype(F32) * (1.0 / HEAD_DIM**0.5)
    for h in range(heads):
        qm[h] = jnp.where(lane_head == h, scaled, 0.0).astype(BF16)
    tri[...] = jnp.where(
        lax.broadcasted_iota(jnp.int32, (kc, kc), 0) > lax.broadcasted_iota(jnp.int32, (kc, kc), 1), 1.0, 0.0
    ).astype(BF16)
    acc_low[...] = jnp.zeros_like(acc_low)
    gall[pl.ds(pl.multiple_of(s * d_rows, d_rows), d_rows), :] = gate_ref[...]
    uall[pl.ds(pl.multiple_of(s * d_rows, d_rows), d_rows), :] = up_ref[...]

    def attend(keys, vals, mode):
        def tile(i, carry_in):
            rows = pl.ds(pl.multiple_of(i * qt, qt), qt)
            for h in range(heads):
                qtile = qm[h, rows, :]
                gone = lost[h, rows, :] if mode == "high" else jnp.zeros((qt, 1), F32)
                out = jnp.zeros((qt, width), F32)
                for c in reversed(range(toks // kc)):
                    z = lax.dot_general(
                        qtile, keys[pl.ds(c * kc, kc), :], (((1,), (1,)), ((), ())), preferred_element_type=F32
                    )
                    soft = jnp.maximum(z, 0.0) + jnp.log(1.0 + jnp.exp2(jnp.abs(z) * -LOG2_E))
                    take = z - soft
                    if mode == "own":
                        key_pos = c * kc + lax.broadcasted_iota(jnp.int32, (qt, kc), 1)
                        strict = key_pos < i * qt + lax.broadcasted_iota(jnp.int32, (qt, kc), 0)
                        soft = jnp.where(strict, soft, 0.0)
                    head = soft.astype(BF16)
                    rest = (soft - head.astype(F32)).astype(BF16)
                    later = jnp.dot(head, tri[...], preferred_element_type=F32) + jnp.dot(
                        rest, tri[...], preferred_element_type=F32
                    )
                    weight = jnp.exp(take - later - gone)
                    if mode == "own":
                        weight = jnp.where(strict, weight, 0.0)
                    out = out + jnp.dot(
                        weight.astype(BF16), vals[pl.ds(c * kc, kc), :], preferred_element_type=F32
                    )
                    gone = gone + later[:, 0:1] + soft[:, 0:1]
                if mode == "own":
                    acc[h, rows, :] = out
                    lost[h, rows, :] = gone
                elif mode == "high":
                    acc[h, rows, :] = acc[h, rows, :] + out
                    lost[h, rows, :] = gone
                else:
                    acc_low[h, rows, :] = acc_low[h, rows, :] * jnp.exp(-gone) + out
            return carry_in

        lax.fori_loop(0, toks // qt, tile, 0)

    attend(k_ref, v_ref, "own")

    def kv_step(k, carry_in):
        up_need = s - 1 - k >= 0
        wrap = lax.rem(s + 1 + k, n)
        down_need = jnp.logical_and(k < near, wrap < near)
        for i in KV:
            @pl.when(up_need)
            def _():
                in_copy(i, 0, k).wait_recv()

                @pl.when(jnp.logical_and(k + 1 < far, s < n - 1))
                def _():
                    out_copy(i, 0, k + 1).start()

            @pl.when(down_need)
            def _():
                in_copy(i, 1, k).wait_recv()

                @pl.when(k + 1 < near)
                def _():
                    out_copy(i, 1, k + 1).start()

        @pl.when(k == far - 2)
        def _():
            start_group(GU)

        @pl.when(k == far - 1)
        def _():
            service(GU, 0)

        @pl.when(up_need)
        def _():
            o = origin_in(0, k)
            attend(kall.at[o], vall.at[o], "high")

        @pl.when(jnp.logical_and(down_need, wrap < s))
        def _():
            attend(kall.at[wrap], vall.at[wrap], "low")

        return carry_in

    lax.fori_loop(0, far, kv_step, 0)

    whole = [acc[h] + acc_low[h] * jnp.exp(-lost[h]) for h in range(heads)]
    joined = whole[0]
    for h in range(1, heads):
        joined = jnp.where(lane_head == h, whole[h], joined)
    att[...] = joined.astype(BF16)
    nc = min(512, d_model)
    for c in range(d_model // nc):
        sbuf[:, pl.ds(c * nc, nc)] = jnp.dot(
            att[...], wo_ref[:, pl.ds(c * nc, nc)], preferred_element_type=F32
        ).astype(BF16)

    n_x = m // 2
    assert n_x == 4
    x, core = me // 2, lax.rem(me, 2)
    x_up, x_far, x_dn = lax.rem(x + 1, n_x), lax.rem(x + 2, n_x), lax.rem(x + 3, n_x)
    mate = {"tp": 2 * x + 1 - core}
    up_dev, dn_dev = {"tp": 2 * x_up + core}, {"tp": 2 * x_dn + core}
    hp = part // 2
    top, bottom = pl.ds(0, hp), pl.ds(hp, hp)

    def rows_of(at_x, at_core, begin=0, size=part):
        return pl.ds(pl.multiple_of((2 * at_x + at_core) * part + begin, size), size)

    order = (x_far, x_up, x_dn, x)

    class Sum:
        def __init__(self, src, pairs, sums, halves, joint, kept, send, recv):
            self.src, self.pairs, self.sums, self.halves, self.joint, self.kept = src, pairs, sums, halves, joint, kept
            self.pair = [rcopy(src(rows_of(order[j], 1 - core)), pairs(j), send(j), recv(j), mate) for j in range(4)]
            self.along = [
                rcopy(sums(0, top), halves(0), send(4), recv(4), up_dev),
                rcopy(sums(0, bottom), halves(1), send(5), recv(5), dn_dev),
                rcopy(sums(1, bottom), halves(2), send(6), recv(6), up_dev),
                rcopy(sums(2, top), halves(3), send(7), recv(7), dn_dev),
                rcopy(joint(0), halves(4), send(8), recv(8), up_dev),
                rcopy(joint(1), halves(5), send(9), recv(9), dn_dev),
            ]

        def to_mate(self):
            for copy in self.pair:
                copy.start()

        def join_pair(self):
            for j in range(4):
                self.pair[j].wait_recv()
                pair = self.src(rows_of(order[j], core))[...].astype(F32) + self.pairs(j)[...].astype(F32)
                if j == 3:
                    self.kept[...] = pair
                else:
                    self.sums(j, pl.ds(0, part))[...] = pair.astype(BF16)
                    for i in ((0, 1), (2,), (3,))[j]:
                        self.along[i].start()

        def pass_far(self):
            for i, j, half in ((0, 1, top), (1, 2, bottom)):
                self.along[i].wait_recv()
                both = self.sums(j, half)[...].astype(F32) + self.halves(i)[...].astype(F32)
                self.joint(i)[...] = both.astype(BF16)
                self.along[4 + i].start()

        def result(self):
            for i in (2, 3, 4, 5):
                self.along[i].wait_recv()
            for half, raw, summed in ((top, 3, 4), (bottom, 2, 5)):
                yield half, self.kept[half, :] + self.halves(raw)[...].astype(F32) + self.halves(summed)[...].astype(F32)

        def sent(self):
            for copy in self.pair + self.along:
                copy.wait_send()

    mix = Sum(
        lambda r: sbuf.at[r, :], lambda j: pbuf.at[j], lambda j, r: tbuf.at[j, r, :], lambda i: hbuf.at[i],
        lambda i: cbuf.at[i], first, lambda i: rs_send.at[i], lambda i: rs_recv.at[i],
    )

    def ag_to(i, at_x, device, begin=0, size=part):
        at = x_all.at[rows_of(at_x, core, begin, size), :]
        return rcopy(at, at, ag_send.at[i], ag_recv.at[i], device)

    def ag_from(i, at_x, at_core, begin=0, size=part):
        at = x_all.at[rows_of(at_x, at_core, begin, size), :]
        return rcopy(at, at, ag_send.at[i], ag_recv.at[i], mate)

    ag_out = [
        ag_to(0, x, up_dev), ag_to(1, x, dn_dev), ag_to(2, x, mate),
        ag_to(3, x_dn, up_dev, 0, hp), ag_to(4, x_dn, mate),
        ag_to(5, x_up, dn_dev, hp, hp), ag_to(6, x_up, mate),
        ag_to(7, x_far, mate, 0, hp), ag_to(8, x_far, mate, hp, hp),
    ]
    ag_in = [
        ag_from(0, x_dn, core), ag_from(1, x_up, core), ag_from(2, x, 1 - core),
        ag_from(3, x_far, core, 0, hp), ag_from(4, x_dn, 1 - core),
        ag_from(5, x_far, core, hp, hp), ag_from(6, x_up, 1 - core),
        ag_from(7, x_far, 1 - core, 0, hp), ag_from(8, x_far, 1 - core, hp, hp),
    ]

    def norm(v, gain):
        mean_square = jnp.mean(v * v, axis=-1, keepdims=True)
        return v * lax.rsqrt(mean_square + norm_eps) * gain

    lag = 2

    def ring_step(j):
        if j < far:
            service(GU, j)
        if j == lag - 1:
            start_group(DN)
        if j >= lag:
            service(DN, j - lag)

    mix.to_mate()
    ring_step(1)
    mix.join_pair()
    ring_step(2)
    mix.pass_far()
    ring_step(3)
    res_copy.wait()
    for half, mixed in mix.result():
        first[half, :] = res_v[half, :].astype(F32) + norm(mixed, pg_ref[...])
    x_all[rows_of(x, core), :] = norm(first[...], prg_ref[...]).astype(BF16)
    for i in (0, 1, 2):
        ag_out[i].start()
    ring_step(4)
    ag_in[0].wait_recv()
    for i in (3, 4):
        ag_out[i].start()
    ag_in[1].wait_recv()
    for i in (5, 6):
        ag_out[i].start()
    ring_step(5)
    ag_in[3].wait_recv()
    ag_out[7].start()
    ag_in[5].wait_recv()
    ag_out[8].start()
    for k in range(6, far):
        ring_step(k)
    done = far - lag
    early = min(far, max(done + 1, cross_hops[0] - 1))
    for k in range(max(early - done, cross_hops[0])):
        if done + k < early:
            service(DN, done + k)
        if k < cross_hops[0]:
            cross_step(k)
    for i in (2, 4, 6, 7, 8):
        ag_in[i].wait_recv()

    mt = min(256, toks)

    def ffn_tile(i, carry_in):
        rows = pl.ds(pl.multiple_of(i * mt, mt), mt)
        g = jnp.dot(x_all[rows, :], gall[...], preferred_element_type=F32)
        u = jnp.dot(x_all[rows, :], uall[...], preferred_element_type=F32)
        hidden[rows, :] = (g / (1.0 + jnp.exp(-g)) * u).astype(BF16)
        return carry_in

    lax.fori_loop(0, toks // mt, ffn_tile, 0)

    def origins_of(c):
        if c == 0:
            return [s]
        return [origin_in(way, c - 1) for way in (0, 1) if c - 1 < streams[DN[0]][2][way]]

    size = -(-(far + 1) // N_COL_GROUPS)
    members = [list(range(i, min(i + size, far + 1))) for i in range(0, far + 1, size)]
    origins = [[o for c in chunk for o in origins_of(c)] for chunk in members]

    def column_sum(q):
        wide = pl.ds(0, cols * len(origins[q]))
        return Sum(
            lambda r: fbuf.at[q, r, wide], lambda j: pb.at[q, j, :, wide], lambda j, r: tb.at[q, j, r, wide],
            lambda i: hb.at[q, i, :, wide], lambda i: cb.at[q, i, :, wide], kept.at[q, :, wide],
            lambda i: fs_send.at[q, i], lambda i: fs_recv.at[q, i],
        )

    col_sums = [column_sum(q) for q in range(len(members))]
    square = [jnp.zeros((hp, 1), F32), jnp.zeros((hp, 1), F32)]
    for step in range(len(members) + 3):
        if step < len(members):
            at = 0
            for c in members[step]:
                if c > early:
                    service(DN, c - 1)
                tiles = [down_ref[...] if c == 0 else dall[o] for o in origins_of(c)]
                both = tiles[0] if len(tiles) == 1 else jnp.concatenate(tiles, axis=1)
                wide = cols * len(tiles)
                fbuf[step, :, pl.ds(at, wide)] = jnp.dot(hidden[...], both, preferred_element_type=F32).astype(BF16)
                at += wide
            col_sums[step].to_mate()
        if 0 <= step - 1 < len(members):
            col_sums[step - 1].join_pair()
        if 0 <= step - 2 < len(members):
            col_sums[step - 2].pass_far()
        if 0 <= step - 3 < len(members):
            for i, (half, total) in enumerate(col_sums[step - 3].result()):
                square[i] = square[i] + jnp.sum(total * total, axis=-1, keepdims=True)
                for j, o in enumerate(origins[step - 3]):
                    ff[o, half, :] = total[:, j * cols : (j + 1) * cols]
    square = jnp.concatenate(square, axis=0)
    scale = lax.rsqrt(square / d_model + norm_eps)
    for o in range(n):
        at = pl.ds(o * cols, cols)
        out_ref[:, at] = (first[:, at] + 0.5 * (ff[o] * scale * fg_ref[:, at])).astype(out_ref.dtype)

    for total in (mix, *col_sums):
        total.sent()
    for copy in ag_out:
        copy.wait_send()

    def kv_drain(k, carry_in):
        for i in KV:
            @pl.when(jnp.logical_and(s < n - 1, s - k >= 0))
            def _():
                out_copy(i, 0, k).wait_send()

            @pl.when(jnp.logical_and(k < near, lax.rem(s + k, n) < near))
            def _():
                out_copy(i, 1, k).wait_send()

        return carry_in

    lax.fori_loop(0, far, kv_drain, 0)
    drain(GU)
    cross_drain()
    drain(DN)


def solution(mesh):
    groups, n, m = mesh.shape["grp"], mesh.shape["sp"], mesh.shape["tp"]

    def per_device(q, k, v, residual, wo, pg, gate, up, down, prg, fg):
        toks, width = q.shape
        d_model = wo.shape[1]
        f_loc = gate.shape[1]
        heads = width // HEAD_DIM
        part = toks // m
        cols = down.shape[1]
        far = n // 2
        size = -(-(far + 1) // N_COL_GROUPS)
        col_groups, wide = -(-(far + 1) // size), 2 * size * cols
        kc = min(256, toks)
        vm, dma = pltpu.VMEM, pltpu.SemaphoreType.DMA
        in_vmem = pl.BlockSpec(memory_space=vm)
        specs = [in_vmem] * 11
        specs[3] = pl.BlockSpec(memory_space=pl.ANY)
        flops = 2 * toks * (n * toks * width * 4 + width * d_model + 3 * d_model * f_loc)
        return pl.pallas_call(
            functools.partial(layer_kernel, groups, n, m),
            out_shape=jax.ShapeDtypeStruct((part, d_model), BF16),
            in_specs=specs,
            out_specs=in_vmem,
            scratch_shapes=[
                vm((n, toks, width), BF16),
                vm((n, toks, width), BF16),
                vm((d_model, f_loc), BF16),
                vm((d_model, f_loc), BF16),
                vm((n, f_loc, cols), BF16),
                vm((heads, toks, width), BF16),
                vm((kc, kc), BF16),
                vm((heads, toks, width), F32),
                vm((heads, toks, width), F32),
                vm((heads, toks, 1), F32),
                vm((toks, width), BF16),
                vm((toks, d_model), BF16),
                vm((4, part, d_model), BF16),
                vm((3, part, d_model), BF16),
                vm((6, part // 2, d_model), BF16),
                vm((2, part // 2, d_model), BF16),
                vm((part, d_model), BF16),
                vm((part, d_model), F32),
                vm((toks, d_model), BF16),
                vm((toks, f_loc), BF16),
                vm((col_groups, toks, wide), BF16),
                vm((col_groups, 4, part, wide), BF16),
                vm((col_groups, 3, part, wide), BF16),
                vm((col_groups, 6, part // 2, wide), BF16),
                vm((col_groups, 2, part // 2, wide), BF16),
                vm((col_groups, part, wide), F32),
                vm((n, part, cols), F32),
                dma((7, 2, far)),
                dma((7, 2, far)),
                dma((2, n // groups, 2, max(1, groups // 2))),
                dma((2, n // groups, 2, max(1, groups // 2))),
                dma((10,)),
                dma((10,)),
                dma((9,)),
                dma((9,)),
                dma((col_groups, 10)),
                dma((col_groups, 10)),
                dma,
            ],
            compiler_params=pltpu.CompilerParams(
                collective_id=0, has_side_effects=True, vmem_limit_bytes=60 * 1024 * 1024
            ),
            cost_estimate=pl.CostEstimate(flops=flops, bytes_accessed=4 * toks * d_model, transcendentals=0),
        )(q, k, v, residual, wo, pg.reshape(1, -1), gate, up, down, prg.reshape(1, -1), fg.reshape(1, -1))

    in_specs = (
        P(("grp", "sp"), "tp"),
        P(("grp", "sp"), "tp"),
        P(("grp", "sp"), "tp"),
        P(("grp", "sp"), None),
        P("tp", None),
        P(),
        P("sp", "tp"),
        P("sp", "tp"),
        P("tp", "sp"),
        P(),
        P(),
    )
    out_specs = P(("grp", "sp", "tp"), None)
    return jax.shard_map(per_device, mesh=mesh, in_specs=in_specs, out_specs=out_specs, check_vma=False)
```

```python
import functools

import jax
import jax.numpy as jnp
from jax import lax
from jax.experimental import pallas as pl
from jax.experimental.pallas import tpu as pltpu
from jax.sharding import PartitionSpec as P

HEAD_DIM = 64
norm_eps = 1e-06
N_COL_GROUPS = 5
LOG2_E = 1.4426950408889634
MESH = pl.DeviceIdType.MESH
F32 = jnp.float32
BF16 = jnp.bfloat16


def rcopy(src, dst, send_sem, recv_sem, device):
    return pltpu.make_async_remote_copy(
        src_ref=src, dst_ref=dst, send_sem=send_sem, recv_sem=recv_sem,
        device_id=device, device_id_type=MESH,
    )


def layer_kernel(
    groups, n, m,
    q_ref, k_ref, v_ref, res_ref, wo_ref, pg_ref, gate_ref, up_ref, down_ref, prg_ref, fg_ref,
    out_ref,
    kall, vall, gall, uall, dall, qm, tri, acc, acc_low, lost, att, sbuf, pbuf, tbuf, hbuf, cbuf, res_v, first, x_all, hidden,
    fbuf, pb, tb, hb, cb, kept, ff,
    ring_send, ring_recv, cross_send, cross_recv, rs_send, rs_recv, ag_send, ag_recv, fs_send, fs_recv, res_sem,
):
    g = lax.axis_index("grp")
    s = lax.axis_index("sp")
    me = lax.axis_index("tp")
    nxt, prv = lax.rem(s + 1, n), lax.rem(s + n - 1, n)
    toks, width = q_ref.shape
    heads = width // HEAD_DIM
    d_rows = gate_ref.shape[0]
    f_half = down_ref.shape[0] // 2
    cols = down_ref.shape[1]
    d_model = wo_ref.shape[1]
    part = toks // m
    kc = min(256, toks)
    qt = min(512, toks)
    near, far = n // 2 - 1, n // 2

    barrier = pltpu.get_barrier_semaphore()
    for z in (nxt, prv):
        pl.semaphore_signal(barrier, inc=1, device_id={"sp": z}, device_id_type=MESH)
    for d in range(1, m):
        pl.semaphore_signal(barrier, inc=1, device_id={"tp": lax.rem(me + d, m)}, device_id_type=MESH)
    sides = sorted({1 % groups, groups - 1} - {0})
    for d in sides:
        pl.semaphore_signal(barrier, inc=1, device_id={"grp": lax.rem(g + d, groups)}, device_id_type=MESH)
    pl.semaphore_wait(barrier, m + 1 + len(sides))

    d_half = d_rows // 2

    def w_rows(ref, begin, size):
        return lambda o: ref.at[pl.ds(pl.multiple_of(o * d_rows + begin, size), size), :]

    streams = [
        (k_ref, lambda o: kall.at[o], (far, near), False),
        (v_ref, lambda o: vall.at[o], (far, near), False),
        (gate_ref, w_rows(gall, 0, d_rows), (near, far), True),
        (up_ref.at[pl.ds(0, d_half), :], w_rows(uall, 0, d_half), (near, far), False),
        (up_ref.at[pl.ds(d_half, d_half), :], w_rows(uall, d_half, d_half), (near, far), True),
        (down_ref.at[pl.ds(0, f_half), :], lambda o: dall.at[o, pl.ds(0, f_half), :], (far, near), False),
        (down_ref.at[pl.ds(f_half, f_half), :], lambda o: dall.at[o, pl.ds(f_half, f_half), :], (far, near), False),
    ]
    split = [i for i, stream in enumerate(streams) if stream[3]]
    cross_hops = (groups // 2, groups - 1 - groups // 2)
    shares = n // groups

    def carried(i, o, act):
        if streams[i][3] and groups > 1:
            pl.when(lax.rem(o, groups) == g)(act)
        else:
            act()

    def cross_copy(i, o, way, k):
        at, j = streams[i][1](o), split.index(i)
        side = lax.rem(g + (1 if way == 0 else groups - 1), groups)
        sems = (j, o // groups, way, k)
        return rcopy(at, at, cross_send.at[sems], cross_recv.at[sems], {"grp": side})

    def cross_class(way, k, incoming):
        hop = k + incoming
        return lax.rem(g + groups - hop, groups) if way == 0 else lax.rem(g + hop, groups)

    def cross_each(i, k, incoming, act):
        for way in (0, 1):
            if k < cross_hops[way]:
                for b in range(shares):
                    o = b * groups + cross_class(way, k, incoming)
                    pl.when(o != s)(functools.partial(act, i, o, way, k))

    def cross_step(k):
        def take(i, o, way, k):
            cross_copy(i, o, way, k).wait_recv()
            if k + 1 < cross_hops[way]:
                cross_copy(i, o, way, k + 1).start()

        for i in split:
            cross_each(i, k, 1, take)

    def cross_drain():
        for i in split:
            for k in range(cross_hops[0]):
                cross_each(i, k, 0, lambda i, o, way, k: cross_copy(i, o, way, k).wait_send())

    def origin_out(way, k):
        return lax.rem(s + n - k, n) if way == 0 else lax.rem(s + k, n)

    def origin_in(way, k):
        return lax.rem(s + n - 1 - k, n) if way == 0 else lax.rem(s + 1 + k, n)

    def out_copy(i, way, k):
        own, place = streams[i][:2]
        at = place(origin_out(way, k))
        src = own if isinstance(k, int) and k == 0 else at
        return rcopy(src, at, ring_send.at[i, way, k], ring_recv.at[i, way, k], {"sp": nxt if way == 0 else prv})

    def in_copy(i, way, k):
        at = streams[i][1](origin_in(way, k))
        return rcopy(at, at, ring_send.at[i, way, k], ring_recv.at[i, way, k], {"sp": prv if way == 0 else nxt})

    def start_group(group):
        for i in group:
            for way in (0, 1):
                if streams[i][2][way]:
                    carried(i, s, out_copy(i, way, 0).start)

    def service(group, k):
        for i in group:
            for way in (0, 1):
                hops = streams[i][2][way]
                if k < hops:
                    o = origin_in(way, k)

                    def pass_on(i=i, way=way, hops=hops, o=o):
                        in_copy(i, way, k).wait_recv()
                        if k + 1 < hops:
                            out_copy(i, way, k + 1).start()
                        if streams[i][3]:
                            for across in (0, 1):
                                if cross_hops[across]:
                                    cross_copy(i, o, across, 0).start()

                    carried(i, o, pass_on)

    def drain(group):
        for i in group:
            for way in (0, 1):
                for k in range(streams[i][2][way]):
                    carried(i, origin_out(way, k), out_copy(i, way, k).wait_send)

    KV, GU, DN = (0, 1), (2, 3, 4), (5, 6)

    @pl.when(s < n - 1)
    def _():
        for i in KV:
            out_copy(i, 0, 0).start()

    @pl.when(s < near)
    def _():
        for i in KV:
            out_copy(i, 1, 0).start()

    res_copy = pltpu.make_async_copy(res_ref.at[pl.ds(pl.multiple_of(me * part, part), part), :], res_v, res_sem)
    res_copy.start()

    lane_head = lax.broadcasted_iota(jnp.int32, (toks, width), 1) // HEAD_DIM
    scaled = q_ref[...].astype(F32) * (1.0 / HEAD_DIM**0.5)
    for h in range(heads):
        qm[h] = jnp.where(lane_head == h, scaled, 0.0).astype(BF16)
    tri[...] = jnp.where(
        lax.broadcasted_iota(jnp.int32, (kc, kc), 0) > lax.broadcasted_iota(jnp.int32, (kc, kc), 1), 1.0, 0.0
    ).astype(BF16)
    acc_low[...] = jnp.zeros_like(acc_low)
    gall[pl.ds(pl.multiple_of(s * d_rows, d_rows), d_rows), :] = gate_ref[...]
    uall[pl.ds(pl.multiple_of(s * d_rows, d_rows), d_rows), :] = up_ref[...]

    def attend(keys, vals, mode):
        def tile(i, carry_in):
            rows = pl.ds(pl.multiple_of(i * qt, qt), qt)
            for h in range(heads):
                qtile = qm[h, rows, :]
                gone = lost[h, rows, :] if mode == "high" else jnp.zeros((qt, 1), F32)
                out = jnp.zeros((qt, width), F32)
                for c in reversed(range(toks // kc)):
                    z = lax.dot_general(
                        qtile, keys[pl.ds(c * kc, kc), :], (((1,), (1,)), ((), ())), preferred_element_type=F32
                    )
                    soft = jnp.maximum(z, 0.0) + jnp.log(1.0 + jnp.exp2(jnp.abs(z) * -LOG2_E))
                    take = z - soft
                    if mode == "own":
                        key_pos = c * kc + lax.broadcasted_iota(jnp.int32, (qt, kc), 1)
                        strict = key_pos < i * qt + lax.broadcasted_iota(jnp.int32, (qt, kc), 0)
                        soft = jnp.where(strict, soft, 0.0)
                    head = soft.astype(BF16)
                    rest = (soft - head.astype(F32)).astype(BF16)
                    later = jnp.dot(head, tri[...], preferred_element_type=F32) + jnp.dot(
                        rest, tri[...], preferred_element_type=F32
                    )
                    weight = jnp.exp(take - later - gone)
                    if mode == "own":
                        weight = jnp.where(strict, weight, 0.0)
                    out = out + jnp.dot(
                        weight.astype(BF16), vals[pl.ds(c * kc, kc), :], preferred_element_type=F32
                    )
                    gone = gone + later[:, 0:1] + soft[:, 0:1]
                if mode == "own":
                    acc[h, rows, :] = out
                    lost[h, rows, :] = gone
                elif mode == "high":
                    acc[h, rows, :] = acc[h, rows, :] + out
                    lost[h, rows, :] = gone
                else:
                    acc_low[h, rows, :] = acc_low[h, rows, :] * jnp.exp(-gone) + out
            return carry_in

        lax.fori_loop(0, toks // qt, tile, 0)

    attend(k_ref, v_ref, "own")

    def kv_step(k, carry_in):
        up_need = s - 1 - k >= 0
        wrap = lax.rem(s + 1 + k, n)
        down_need = jnp.logical_and(k < near, wrap < near)
        for i in KV:
            @pl.when(up_need)
            def _():
                in_copy(i, 0, k).wait_recv()

                @pl.when(jnp.logical_and(k + 1 < far, s < n - 1))
                def _():
                    out_copy(i, 0, k + 1).start()

            @pl.when(down_need)
            def _():
                in_copy(i, 1, k).wait_recv()

                @pl.when(k + 1 < near)
                def _():
                    out_copy(i, 1, k + 1).start()

        @pl.when(k == far - 2)
        def _():
            start_group(GU)

        @pl.when(k == far - 1)
        def _():
            service(GU, 0)

        @pl.when(up_need)
        def _():
            o = origin_in(0, k)
            attend(kall.at[o], vall.at[o], "high")

        @pl.when(jnp.logical_and(down_need, wrap < s))
        def _():
            attend(kall.at[wrap], vall.at[wrap], "low")

        return carry_in

    lax.fori_loop(0, far, kv_step, 0)

    whole = [acc[h] + acc_low[h] * jnp.exp(-lost[h]) for h in range(heads)]
    joined = whole[0]
    for h in range(1, heads):
        joined = jnp.where(lane_head == h, whole[h], joined)
    att[...] = joined.astype(BF16)
    nc = min(512, d_model)
    for c in range(d_model // nc):
        sbuf[:, pl.ds(c * nc, nc)] = jnp.dot(
            att[...], wo_ref[:, pl.ds(c * nc, nc)], preferred_element_type=F32
        ).astype(BF16)

    n_x = m // 2
    assert n_x == 4
    x, core = me // 2, lax.rem(me, 2)
    x_up, x_far, x_dn = lax.rem(x + 1, n_x), lax.rem(x + 2, n_x), lax.rem(x + 3, n_x)
    mate = {"tp": 2 * x + 1 - core}
    up_dev, dn_dev = {"tp": 2 * x_up + core}, {"tp": 2 * x_dn + core}
    hp = part // 2
    top, bottom = pl.ds(0, hp), pl.ds(hp, hp)

    def rows_of(at_x, at_core, begin=0, size=part):
        return pl.ds(pl.multiple_of((2 * at_x + at_core) * part + begin, size), size)

    order = (x_far, x_up, x_dn, x)

    class Sum:
        def __init__(self, src, pairs, sums, halves, joint, kept, send, recv):
            self.src, self.pairs, self.sums, self.halves, self.joint, self.kept = src, pairs, sums, halves, joint, kept
            self.pair = [rcopy(src(rows_of(order[j], 1 - core)), pairs(j), send(j), recv(j), mate) for j in range(4)]
            self.along = [
                rcopy(sums(0, top), halves(0), send(4), recv(4), up_dev),
                rcopy(sums(0, bottom), halves(1), send(5), recv(5), dn_dev),
                rcopy(sums(1, bottom), halves(2), send(6), recv(6), up_dev),
                rcopy(sums(2, top), halves(3), send(7), recv(7), dn_dev),
                rcopy(joint(0), halves(4), send(8), recv(8), up_dev),
                rcopy(joint(1), halves(5), send(9), recv(9), dn_dev),
            ]

        def to_mate(self):
            for copy in self.pair:
                copy.start()

        def join_pair(self):
            for j in range(4):
                self.pair[j].wait_recv()
                pair = self.src(rows_of(order[j], core))[...].astype(F32) + self.pairs(j)[...].astype(F32)
                if j == 3:
                    self.kept[...] = pair
                else:
                    self.sums(j, pl.ds(0, part))[...] = pair.astype(BF16)
                    for i in ((0, 1), (2,), (3,))[j]:
                        self.along[i].start()

        def pass_far(self):
            for i, j, half in ((0, 1, top), (1, 2, bottom)):
                self.along[i].wait_recv()
                both = self.sums(j, half)[...].astype(F32) + self.halves(i)[...].astype(F32)
                self.joint(i)[...] = both.astype(BF16)
                self.along[4 + i].start()

        def result(self):
            for i in (2, 3, 4, 5):
                self.along[i].wait_recv()
            for half, raw, summed in ((top, 3, 4), (bottom, 2, 5)):
                yield half, self.kept[half, :] + self.halves(raw)[...].astype(F32) + self.halves(summed)[...].astype(F32)

        def sent(self):
            for copy in self.pair + self.along:
                copy.wait_send()

    mix = Sum(
        lambda r: sbuf.at[r, :], lambda j: pbuf.at[j], lambda j, r: tbuf.at[j, r, :], lambda i: hbuf.at[i],
        lambda i: cbuf.at[i], first, lambda i: rs_send.at[i], lambda i: rs_recv.at[i],
    )

    def ag_to(i, at_x, device, begin=0, size=part):
        at = x_all.at[rows_of(at_x, core, begin, size), :]
        return rcopy(at, at, ag_send.at[i], ag_recv.at[i], device)

    def ag_from(i, at_x, at_core, begin=0, size=part):
        at = x_all.at[rows_of(at_x, at_core, begin, size), :]
        return rcopy(at, at, ag_send.at[i], ag_recv.at[i], mate)

    ag_out = [
        ag_to(0, x, up_dev), ag_to(1, x, dn_dev), ag_to(2, x, mate),
        ag_to(3, x_dn, up_dev, 0, hp), ag_to(4, x_dn, mate),
        ag_to(5, x_up, dn_dev, hp, hp), ag_to(6, x_up, mate),
        ag_to(7, x_far, mate, 0, hp), ag_to(8, x_far, mate, hp, hp),
    ]
    ag_in = [
        ag_from(0, x_dn, core), ag_from(1, x_up, core), ag_from(2, x, 1 - core),
        ag_from(3, x_far, core, 0, hp), ag_from(4, x_dn, 1 - core),
        ag_from(5, x_far, core, hp, hp), ag_from(6, x_up, 1 - core),
        ag_from(7, x_far, 1 - core, 0, hp), ag_from(8, x_far, 1 - core, hp, hp),
    ]

    def norm(v, gain):
        mean_square = jnp.mean(v * v, axis=-1, keepdims=True)
        return v * lax.rsqrt(mean_square + norm_eps) * gain

    lag = 3

    def ring_step(j):
        if j < far:
            service(GU, j)
        if j == lag - 1:
            start_group(DN)
        if j >= lag:
            service(DN, j - lag)

    mix.to_mate()
    ring_step(1)
    mix.join_pair()
    ring_step(2)
    mix.pass_far()
    ring_step(3)
    res_copy.wait()
    for half, mixed in mix.result():
        first[half, :] = res_v[half, :].astype(F32) + norm(mixed, pg_ref[...])
    x_all[rows_of(x, core), :] = norm(first[...], prg_ref[...]).astype(BF16)
    for i in (0, 1, 2):
        ag_out[i].start()
    ring_step(4)
    ag_in[0].wait_recv()
    for i in (3, 4):
        ag_out[i].start()
    ag_in[1].wait_recv()
    for i in (5, 6):
        ag_out[i].start()
    ring_step(5)
    ag_in[3].wait_recv()
    ag_out[7].start()
    ag_in[5].wait_recv()
    ag_out[8].start()
    for k in range(6, far):
        ring_step(k)
    done = far - lag
    early = min(far, max(done + 1, cross_hops[0] - 1))
    for k in range(max(early - done, cross_hops[0])):
        if done + k < early:
            service(DN, done + k)
        if k < cross_hops[0]:
            cross_step(k)
    for i in (2, 4, 6, 7, 8):
        ag_in[i].wait_recv()

    mt = min(256, toks)

    def ffn_tile(i, carry_in):
        rows = pl.ds(pl.multiple_of(i * mt, mt), mt)
        g = jnp.dot(x_all[rows, :], gall[...], preferred_element_type=F32)
        u = jnp.dot(x_all[rows, :], uall[...], preferred_element_type=F32)
        hidden[rows, :] = (g / (1.0 + jnp.exp(-g)) * u).astype(BF16)
        return carry_in

    lax.fori_loop(0, toks // mt, ffn_tile, 0)

    def origins_of(c):
        if c == 0:
            return [s]
        return [origin_in(way, c - 1) for way in (0, 1) if c - 1 < streams[DN[0]][2][way]]

    size = -(-(far + 1) // N_COL_GROUPS)
    members = [list(range(i, min(i + size, far + 1))) for i in range(0, far + 1, size)]
    origins = [[o for c in chunk for o in origins_of(c)] for chunk in members]

    def column_sum(q):
        wide = pl.ds(0, cols * len(origins[q]))
        return Sum(
            lambda r: fbuf.at[q, r, wide], lambda j: pb.at[q, j, :, wide], lambda j, r: tb.at[q, j, r, wide],
            lambda i: hb.at[q, i, :, wide], lambda i: cb.at[q, i, :, wide], kept.at[q, :, wide],
            lambda i: fs_send.at[q, i], lambda i: fs_recv.at[q, i],
        )

    col_sums = [column_sum(q) for q in range(len(members))]
    square = [jnp.zeros((hp, 1), F32), jnp.zeros((hp, 1), F32)]
    for step in range(len(members) + 3):
        if step < len(members):
            at = 0
            for c in members[step]:
                if c > early:
                    service(DN, c - 1)
                tiles = [down_ref[...] if c == 0 else dall[o] for o in origins_of(c)]
                both = tiles[0] if len(tiles) == 1 else jnp.concatenate(tiles, axis=1)
                wide = cols * len(tiles)
                fbuf[step, :, pl.ds(at, wide)] = jnp.dot(hidden[...], both, preferred_element_type=F32).astype(BF16)
                at += wide
            col_sums[step].to_mate()
        if 0 <= step - 1 < len(members):
            col_sums[step - 1].join_pair()
        if 0 <= step - 2 < len(members):
            col_sums[step - 2].pass_far()
        if 0 <= step - 3 < len(members):
            for i, (half, total) in enumerate(col_sums[step - 3].result()):
                square[i] = square[i] + jnp.sum(total * total, axis=-1, keepdims=True)
                for j, o in enumerate(origins[step - 3]):
                    ff[o, half, :] = total[:, j * cols : (j + 1) * cols]
    square = jnp.concatenate(square, axis=0)
    scale = lax.rsqrt(square / d_model + norm_eps)
    for o in range(n):
        at = pl.ds(o * cols, cols)
        out_ref[:, at] = (first[:, at] + 0.5 * (ff[o] * scale * fg_ref[:, at])).astype(out_ref.dtype)

    for total in (mix, *col_sums):
        total.sent()
    for copy in ag_out:
        copy.wait_send()

    def kv_drain(k, carry_in):
        for i in KV:
            @pl.when(jnp.logical_and(s < n - 1, s - k >= 0))
            def _():
                out_copy(i, 0, k).wait_send()

            @pl.when(jnp.logical_and(k < near, lax.rem(s + k, n) < near))
            def _():
                out_copy(i, 1, k).wait_send()

        return carry_in

    lax.fori_loop(0, far, kv_drain, 0)
    drain(GU)
    cross_drain()
    drain(DN)


def solution(mesh):
    groups, n, m = mesh.shape["grp"], mesh.shape["sp"], mesh.shape["tp"]

    def per_device(q, k, v, residual, wo, pg, gate, up, down, prg, fg):
        toks, width = q.shape
        d_model = wo.shape[1]
        f_loc = gate.shape[1]
        heads = width // HEAD_DIM
        part = toks // m
        cols = down.shape[1]
        far = n // 2
        size = -(-(far + 1) // N_COL_GROUPS)
        col_groups, wide = -(-(far + 1) // size), 2 * size * cols
        kc = min(256, toks)
        vm, dma = pltpu.VMEM, pltpu.SemaphoreType.DMA
        in_vmem = pl.BlockSpec(memory_space=vm)
        specs = [in_vmem] * 11
        specs[3] = pl.BlockSpec(memory_space=pl.ANY)
        flops = 2 * toks * (n * toks * width * 4 + width * d_model + 3 * d_model * f_loc)
        return pl.pallas_call(
            functools.partial(layer_kernel, groups, n, m),
            out_shape=jax.ShapeDtypeStruct((part, d_model), BF16),
            in_specs=specs,
            out_specs=in_vmem,
            scratch_shapes=[
                vm((n, toks, width), BF16),
                vm((n, toks, width), BF16),
                vm((d_model, f_loc), BF16),
                vm((d_model, f_loc), BF16),
                vm((n, f_loc, cols), BF16),
                vm((heads, toks, width), BF16),
                vm((kc, kc), BF16),
                vm((heads, toks, width), F32),
                vm((heads, toks, width), F32),
                vm((heads, toks, 1), F32),
                vm((toks, width), BF16),
                vm((toks, d_model), BF16),
                vm((4, part, d_model), BF16),
                vm((3, part, d_model), BF16),
                vm((6, part // 2, d_model), BF16),
                vm((2, part // 2, d_model), BF16),
                vm((part, d_model), BF16),
                vm((part, d_model), F32),
                vm((toks, d_model), BF16),
                vm((toks, f_loc), BF16),
                vm((col_groups, toks, wide), BF16),
                vm((col_groups, 4, part, wide), BF16),
                vm((col_groups, 3, part, wide), BF16),
                vm((col_groups, 6, part // 2, wide), BF16),
                vm((col_groups, 2, part // 2, wide), BF16),
                vm((col_groups, part, wide), F32),
                vm((n, part, cols), F32),
                dma((7, 2, far)),
                dma((7, 2, far)),
                dma((2, n // groups, 2, max(1, groups // 2))),
                dma((2, n // groups, 2, max(1, groups // 2))),
                dma((10,)),
                dma((10,)),
                dma((9,)),
                dma((9,)),
                dma((col_groups, 10)),
                dma((col_groups, 10)),
                dma,
            ],
            compiler_params=pltpu.CompilerParams(
                collective_id=0, has_side_effects=True, vmem_limit_bytes=60 * 1024 * 1024
            ),
            cost_estimate=pl.CostEstimate(flops=flops, bytes_accessed=4 * toks * d_model, transcendentals=0),
        )(q, k, v, residual, wo, pg.reshape(1, -1), gate, up, down, prg.reshape(1, -1), fg.reshape(1, -1))

    in_specs = (
        P(("grp", "sp"), "tp"),
        P(("grp", "sp"), "tp"),
        P(("grp", "sp"), "tp"),
        P(("grp", "sp"), None),
        P("tp", None),
        P(),
        P("sp", "tp"),
        P("sp", "tp"),
        P("tp", "sp"),
        P(),
        P(),
    )
    out_specs = P(("grp", "sp", "tp"), None)
    return jax.shard_map(per_device, mesh=mesh, in_specs=in_specs, out_specs=out_specs, check_vma=False)
```
